32 devices in a mesh: grp: 2 (over x), ep: 8 (over z, y), tp: 2 (over core).
Axes of the slice: x: 2, y: 2, z: 4, core: 2. Of those that a mesh axis runs over, the one named last changes fastest.
Arguments:
- tokens: bfloat16 [8192, 2048], P(('grp', 'ep', 'tp')), parts along dimension 0, may hold values from -6 to 6
- norm_gain: float32 [2048], replicated, may hold values from 0.1 to 1.9
- routes: int32 [8192, 3], P(('grp', 'ep', 'tp')), parts along dimension 0, may hold values from 0 to 7, all different within a row; in each aligned block of 256 rows (0 to 255, 256 to 511, ...) at most 144 rows name the same one
- gates: float32 [8192, 3], P(('grp', 'ep', 'tp')), parts along dimension 0, may hold values from 0.2 to 1.2
- expert_gate: bfloat16 [8, 2048, 512], P('ep', None, 'tp'), may hold values from -0.125 to 0.125
- expert_up: bfloat16 [8, 2048, 512], P('ep', None, 'tp'), may hold values from -0.125 to 0.125
- expert_down: bfloat16 [8, 512, 2048], P('ep', 'tp'), may hold values from -0.25 to 0.25
- shared_gate: bfloat16 [2048, 512], replicated, may hold values from -0.125 to 0.125
- shared_up: bfloat16 [2048, 512], replicated, may hold values from -0.125 to 0.125
- shared_down: bfloat16 [512, 2048], replicated, may hold values from -0.25 to 0.25
Outputs:
- mixed: bfloat16 [8192, 2048], P(('grp', 'ep', 'tp')), parts along dimension 0
The draws below stay inside these ranges and needn't reach their ends.
There are 2 independent parts, one for each index of `grp`. The reference program is written for one: setup_inputs(seed, part) draws one part's arguments, and reference() takes and returns one part's arrays. A program takes and returns all parts, laid end to end along the dimension named above; an argument that names none is the same for every part. Nothing has to cross between parts.
Inputs may be any that keep to these rules, and one draw needn't show every extreme that they name: `routes`: A row names 3 different experts. Among the rows of one device no expert is named by more than 144 rows, and in every draw some expert is named by exactly 144 rows of some device.
All inputs are finite; a program needn't handle non-finite values.
Results may differ from the reference program's by a relative error of at most 0.01.
Values may be sent and summed in bfloat16 or wider, within the bound.
A program may use at most 128 MiB of HBM per device.

```python
import math
import jax
import jax.numpy as jnp
import numpy as np
from jax import lax

D = 2048
FE = 512
SH_FE = 512
TOP = 3
TOK_DEV = 256
EXPERTS = 8
CAP = 144
TOKENS = 4096
N_EP = 8
N_TP = 2


def level_of(stream_key, extent, pieces, low, top_value):
    factor_of = 1.0
    for dim, parts in pieces:
        draws = jax.random.uniform(jax.random.fold_in(jax.random.fold_in(stream_key, 6), dim), (parts,), jnp.float32, low / len(pieces), top_value / len(pieces))
        factor_of = factor_of * jnp.repeat(jnp.exp(draws), extent[dim] // parts).reshape((-1,) + (1,) * (len(extent) - 1 - dim))
    return factor_of


def routed_block(rng, own, number, rows, number_of, top, limit, skew):
    order = jax.random.permutation(rng, number_of)
    crowded, common = shares(number_of, rows * top, limit, skew, True), shares(number_of, rows * top, limit, skew, False)
    places = jnp.arange(number_of)

    def named(lengths, turn):
        used = int((lengths > 0).sum())
        fixed = max(1, used // 4)
        moved = fixed + (places - fixed + turn * (used - fixed)) % max(1, number_of - fixed)
        return jnp.zeros((number_of,), jnp.int32).at[order[jnp.where(places < fixed, places, moved)]].set(jnp.asarray(lengths, jnp.int32))

    lengths = jnp.where(number % 4 == 0, named(crowded, number // 4), named(common, number - number // 4 - 1))
    mixed = jax.random.permutation(jax.random.fold_in(own, 3), number_of)
    donor, taker = mixed[0:number_of // 2 * 2:2], mixed[1:number_of // 2 * 2:2]
    margin = jnp.minimum(lengths[donor] - 1, limit - lengths[taker]) // 2
    margin = jnp.where((donor == order[0]) | (taker == order[0]) | (lengths[taker] == 0), 0, jnp.maximum(margin, 0))
    moved = jax.random.randint(jax.random.fold_in(own, 4), (number_of // 2,), 0, 1 << 20) % (margin + 1)
    lengths = lengths.at[donor].add(-moved).at[taker].add(moved)
    labels = jnp.searchsorted(jnp.cumsum(lengths), jnp.arange(rows * top), side="right").astype(jnp.int32)
    listing = labels.reshape(top, rows).T
    listing = listing[jax.random.permutation(jax.random.fold_in(own, 1), rows)]
    turn = jax.random.randint(jax.random.fold_in(own, 2), (rows, 1), 0, top)
    return jnp.take_along_axis(listing, (jnp.arange(top)[None, :] + turn) % top, axis=1)


def shares(count, total, limit, skew, full):
    loads = [(1 << 20) // math.isqrt(rank ** skew) + 1 for rank in range(1, count + 1)]
    largest = limit if full else min(limit, max(-(-total // count), total * loads[0] // sum(loads)))
    least = 1 if total - largest >= count - 1 else 0
    given, spare = [largest] + [least] * (count - 1), total - largest - least * (count - 1)
    while spare > 0:
        free = [i for i in range(1, count) if given[i] < largest] or [i for i in range(1, count) if given[i] < limit]
        pool, left = sum([loads[i] for i in free]), spare
        for i in free:
            addition = min(limit - given[i], max(1, left * loads[i] // pool), spare)
            given[i] = given[i] + addition
            spare = spare - addition
    return np.array(given)


def scatter_about(stream_key, dims, deviation, limit, split=(), kind=jnp.bfloat16):
    array = jax.random.normal(stream_key, dims, jnp.float32) * deviation
    if len(split) > 0:
        array = level_of(stream_key, dims, split, -0.22, 0.18) * array
    return jnp.clip(array, min=-limit, max=limit).astype(kind)


def setup_inputs(seed: int = 0, part: int = 0) -> dict:
    splits = jax.random.split(jax.random.key(seed), 11)
    own_keys = jax.random.split(jax.random.fold_in(splits[10], part), 11)
    tokens = scatter_about(own_keys[0], (TOKENS, D), 1.0, 6.0, ((0, 16),))
    norm_gain = jnp.clip(1.0 + 0.18 * jax.random.normal(splits[1], (D,), jnp.float32), 0.1, 1.9)
    routes_keys = jax.random.split(jax.random.fold_in(own_keys[2], 1), TOKENS // TOK_DEV)
    routes_turns = jax.random.permutation(jax.random.fold_in(own_keys[2], 3), TOKENS // TOK_DEV)
    routes = jax.vmap(lambda own, number: routed_block(jax.random.fold_in(own_keys[2], 2), own, number, TOK_DEV, EXPERTS, TOP, CAP, 2))(routes_keys, routes_turns).reshape((TOKENS, TOP))
    gates = jnp.clip(0.2 + 1 * jax.random.uniform(own_keys[3], (TOKENS, TOP), jnp.float32) ** level_of(own_keys[3], (TOKENS, TOP), ((0, 16),), -0.2, 0.2), 0.2, 1.2)
    expert_gate = scatter_about(splits[4], (EXPERTS, D, FE), D ** -0.5, 0.125, ((0, 8), (2, 2)))
    expert_up = scatter_about(splits[5], (EXPERTS, D, FE), D ** -0.5, 0.125, ((0, 8), (2, 2)))
    expert_down = scatter_about(splits[6], (EXPERTS, FE, D), FE ** -0.5, 0.25, ((0, 8), (1, 2)))
    shared_gate = scatter_about(splits[7], (D, SH_FE), D ** -0.5, 0.125)
    shared_up = scatter_about(splits[8], (D, SH_FE), D ** -0.5, 0.125)
    shared_down = scatter_about(splits[9], (SH_FE, D), SH_FE ** -0.5, 0.25)
    return {"tokens": tokens, "norm_gain": norm_gain, "routes": routes, "gates": gates, "expert_gate": expert_gate, "expert_up": expert_up, "expert_down": expert_down, "shared_gate": shared_gate, "shared_up": shared_up, "shared_down": shared_down}


def reference(tokens, norm_gain, routes, gates, expert_gate, expert_up, expert_down, shared_gate, shared_up, shared_down):
    values = tokens.astype(jnp.float32)
    scaling = lax.rsqrt(lax.optimization_barrier(jnp.mean(values * values, axis=1, keepdims=True)) + 1e-06)
    normed = (values * scaling * norm_gain[None, :]).astype(jnp.bfloat16)
    shared_hidden = (jax.nn.silu(jnp.dot(normed, shared_gate, preferred_element_type=jnp.float32)) * jnp.dot(normed, shared_up, preferred_element_type=jnp.float32)).astype(jnp.bfloat16)
    shared_out = jnp.dot(shared_hidden, shared_down, preferred_element_type=jnp.float32)
    token_count = tokens.shape[0]
    top_count = routes.shape[1]
    flat_routes = routes.reshape(-1)
    bound = N_EP * N_TP * CAP
    padded = jnp.concatenate([normed, jnp.zeros((1, D), jnp.bfloat16)], axis=0)
    weights = jnp.concatenate([gates.reshape(-1), jnp.zeros((1,), jnp.float32)], axis=0)

    def one_expert(totals, expert_index):
        picks = jnp.nonzero(flat_routes == expert_index, size=bound, fill_value=token_count * top_count)[0].astype(jnp.int32)
        owners = (picks // top_count).astype(jnp.int32)
        chosen = padded[owners]
        hidden = (jax.nn.silu(jnp.dot(chosen, expert_gate[expert_index], preferred_element_type=jnp.float32)) * jnp.dot(chosen, expert_up[expert_index], preferred_element_type=jnp.float32)).astype(jnp.bfloat16)
        result = jnp.dot(hidden, expert_down[expert_index], preferred_element_type=jnp.float32).astype(jnp.bfloat16)
        weighted = result.astype(jnp.float32) * weights[picks][:, None]
        return (totals.at[owners].add(weighted), None)
    start_totals = jnp.zeros((token_count + 1, D), jnp.float32)
    totals, _ = lax.scan(one_expert, start_totals, jnp.arange(EXPERTS, dtype=jnp.int32))
    return (shared_out + totals[:token_count]).astype(jnp.bfloat16)
```

```python
import functools

import jax
import jax.numpy as jnp
from jax import lax
from jax.experimental import pallas as pl
from jax.experimental.pallas import tpu as pltpu
from jax.sharding import PartitionSpec as P

MESH = pl.DeviceIdType.MESH


def exchange_kernel(
    line,
    tok,
    gain,
    wcol,
    eg,
    eu,
    ed,
    sg,
    su,
    sd,
    out,
    gathered,
    G,
    U,
    D,
    SG,
    SU,
    SD,
    xn,
    hid,
    acc,
    stage,
    land,
    loc_sem,
    ag_send,
    ag_recv,
    w_send,
    w_recv,
    rs_send,
    rs_recv,
):
    rows, width = tok.shape
    half = eg.shape[1]
    shared_width = sg.shape[1]
    last = line - 1
    ep = lax.axis_index("ep")
    z, y = ep // 2, ep % 2
    c = lax.axis_index("tp")
    g = lax.axis_index("grp")
    to_next, to_prev = {"ep": ep + 2}, {"ep": ep - 2}
    to_pair = {"ep": z * 2 + (1 - y)}
    to_core = {"tp": 1 - c}
    to_grp = {"grp": 1 - g}

    barrier = pltpu.get_barrier_semaphore()
    for peer in (to_pair, to_core, to_grp):
        pl.semaphore_signal(barrier, inc=1, device_id=peer, device_id_type=MESH)

    @pl.when(z < last)
    def _():
        pl.semaphore_signal(barrier, inc=1, device_id=to_next, device_id_type=MESH)

    @pl.when(z > 0)
    def _():
        pl.semaphore_signal(barrier, inc=1, device_id=to_prev, device_id_type=MESH)

    locals_ = [
        pltpu.make_async_copy(tok, gathered.at[z], loc_sem.at[0]),
        pltpu.make_async_copy(sg, SG, loc_sem.at[1]),
        pltpu.make_async_copy(su, SU, loc_sem.at[2]),
        pltpu.make_async_copy(sd, SD, loc_sem.at[3]),
        pltpu.make_async_copy(eg, G.at[0], loc_sem.at[4]),
        pltpu.make_async_copy(eu, U.at[0], loc_sem.at[5]),
        pltpu.make_async_copy(ed, D.at[pl.ds(0, half)], loc_sem.at[6]),
    ]
    for copy in locals_:
        copy.start()
    between = jnp.logical_and(z > 0, z < last)

    @pl.when(between)
    def _():
        pl.semaphore_wait(barrier, 5)

    @pl.when(jnp.logical_not(between))
    def _():
        pl.semaphore_wait(barrier, 4)

    def remote(src, dst, send, recv, peer):
        return pltpu.make_async_remote_copy(
            src_ref=src,
            dst_ref=dst,
            send_sem=send,
            recv_sem=recv,
            device_id=peer,
            device_id_type=MESH,
        )

    def ag_copy(way, step):
        block = z - step if way == 0 else z + step
        src = tok if step == 0 else gathered.at[block]
        peer = to_next if way == 0 else to_prev
        return remote(
            src, gathered.at[block], ag_send.at[way, step], ag_recv.at[way, step], peer
        )

    def ag_sends(way, step):
        if way == 0:
            return jnp.logical_and(z - step >= 0, z < last)
        return jnp.logical_and(z + step <= last, z > 0)

    def ag_arrival(way, step):
        block = z - 1 - step if way == 0 else z + 1 + step
        slot = gathered.at[block]
        peer = to_next if way == 0 else to_prev
        return remote(slot, slot, ag_send.at[way, step], ag_recv.at[way, step], peer)

    def ag_arrives(way, step):
        return z - 1 - step >= 0 if way == 0 else z + 1 + step <= last

    def ag_start(step):
        for way in range(2):

            @pl.when(ag_sends(way, step))
            def _():
                ag_copy(way, step).start()

    def ag_wait(step):
        for way in range(2):

            @pl.when(ag_arrives(way, step))
            def _():
                ag_arrival(way, step).wait_recv()

    def piece(k, unit, part):
        if k == 2:
            if part is None:
                return D.at[pl.ds(unit * half, half)]
            n = half // 2
            return D.at[pl.ds(pl.multiple_of(unit * half + part * n, n), n)]
        whole = (G, U)[k].at[unit]
        if part is None:
            return whole
        n = width // 2
        return whole.at[pl.ds(pl.multiple_of(part * n, n), n)]

    own = (eg, eu, ed)

    def own_part(k):
        n = own[k].shape[0] // 2
        return own[k].at[pl.ds(pl.multiple_of(g * n, n), n)]

    def w_copy(kind, k):
        sems = (w_send.at[kind, k], w_recv.at[kind, k])
        if kind == 0:
            return remote(own[k], piece(k, 1, None), *sems, to_core)
        if kind == 1:
            return remote(own_part(k), piece(k, 2, g), *sems, to_pair)
        if kind == 2:
            return remote(piece(k, 2, g), piece(k, 2, g), *sems, to_grp)
        if kind == 3:
            return remote(piece(k, 2, g), piece(k, 3, g), *sems, to_core)
        return remote(piece(k, 2, 1 - g), piece(k, 3, 1 - g), *sems, to_core)

    def w_arrival(kind, k):
        if kind != 2:
            return w_copy(kind, k)
        slot = piece(k, 2, 1 - g)
        return remote(slot, slot, w_send.at[kind, k], w_recv.at[kind, k], to_grp)

    ag_start(0)
    for k in range(3):
        w_copy(1, k).start()
    for k in range(3):
        w_copy(0, k).start()

    tile = 32

    def normalise(block):
        @pl.loop(0, rows // tile)
        def _(i):
            part = pl.ds(pl.multiple_of(i * tile, tile), tile)
            values = gathered[block, part, :].astype(jnp.float32)
            scaling = lax.rsqrt(jnp.mean(values * values, axis=1, keepdims=True) + 1e-06)
            xn[part, :] = (values * scaling * gain[...]).astype(jnp.bfloat16)

    def act(a, b):
        return a / (1.0 + jnp.exp(-a)) * b

    cols_n = 512 if width % 512 == 0 else width

    def over_columns(fn):
        @pl.loop(0, width // cols_n)
        def _(i):
            fn(pl.ds(pl.multiple_of(i * cols_n, cols_n), cols_n))

    def routed(block, fn):
        normalise(block)

        @pl.loop(0, 4)
        def _(u):
            a = jnp.dot(xn[...], G[u], preferred_element_type=jnp.float32)
            b = jnp.dot(xn[...], U[u], preferred_element_type=jnp.float32)
            w = jnp.where(u < 2, wcol[block, :, 0:1], wcol[block, :, 1:2])
            hid[:, pl.ds(pl.multiple_of(u * half, half), half)] = (act(a, b) * w).astype(
                jnp.bfloat16
            )

        over_columns(
            lambda cols: fn(
                cols,
                jnp.dot(
                    hid[:, 0 : 4 * half], D[:, cols], preferred_element_type=jnp.float32
                ),
            )
        )

    locals_[0].wait()
    normalise(z)
    for copy in locals_[1:4]:
        copy.wait()

    @pl.loop(0, shared_width // half)
    def _(u):
        part = pl.ds(pl.multiple_of(u * half, half), half)
        a = jnp.dot(xn[...], SG[:, part], preferred_element_type=jnp.float32)
        b = jnp.dot(xn[...], SU[:, part], preferred_element_type=jnp.float32)
        hid[:, part] = act(a, b).astype(jnp.bfloat16)

    def shared_store(cols):
        acc[:, cols] = jnp.dot(
            hid[:, 0:shared_width], SD[:, cols], preferred_element_type=jnp.float32
        )

    over_columns(shared_store)

    def pass_on(k):
        w_arrival(1, k).wait_recv()
        w_copy(2, k).start()
        w_copy(3, k).start()

    def pass_over(k):
        w_arrival(2, k).wait_recv()
        w_copy(4, k).start()

    pass_on(0)
    pass_on(1)
    ag_wait(0)
    if last > 1:
        ag_start(1)
    pass_over(0)
    pass_on(2)
    pass_over(1)
    pass_over(2)
    for copy in locals_[4:]:
        copy.wait()
    for kind in (0, 3, 4):
        for k in range(3):
            w_arrival(kind, k).wait_recv()

    def add_own(cols, value):
        acc[:, cols] += value

    routed(z, add_own)

    def rs_sends(way, t):
        return jnp.logical_and(z <= t, z < last) if way == 0 else jnp.logical_and(
            last - z <= t, z > 0
        )

    def partial(t):
        for way in range(2):

            @pl.when(rs_sends(way, t))
            def _():
                block = last - t + z if way == 0 else z - last + t

                def store(cols, value):
                    stage[way, t, :, cols] = value.astype(jnp.bfloat16)

                routed(block, store)

    def rs_copy(way, t):
        peer = to_next if way == 0 else to_prev
        return remote(
            stage.at[way, t], land.at[way, t], rs_send.at[way, t], rs_recv.at[way, t], peer
        )

    def over_rows(fn):
        @pl.loop(0, rows // tile)
        def _(i):
            fn(pl.ds(pl.multiple_of(i * tile, tile), tile))

    for t in reversed(range(last)):
        step = last - 1 - t
        if step > 0:
            ag_wait(step)
            if step + 1 < last:
                ag_start(step + 1)
        partial(t)

    for t in range(last):
        for way in range(2):

            @pl.when(rs_sends(way, t))
            def _():
                if t > 0:
                    inner = z > 0 if way == 0 else z < last

                    @pl.when(inner)
                    def _():
                        rs_copy(way, t - 1).wait_recv()

                        def add(part):
                            stage[way, t, part, :] = (
                                stage[way, t, part, :].astype(jnp.float32)
                                + land[way, t - 1, part, :].astype(jnp.float32)
                            ).astype(jnp.bfloat16)

                        over_rows(add)

                rs_copy(way, t).start()

    for way in range(2):

        @pl.when(z > 0 if way == 0 else z < last)
        def _():
            rs_copy(way, last - 1).wait_recv()

            def add(part):
                acc[part, :] += land[way, last - 1, part, :].astype(jnp.float32)

            over_rows(add)

    def finish(part):
        out[part, :] = acc[part, :].astype(jnp.bfloat16)

    over_rows(finish)

    for kind in range(5):
        for k in range(3):
            w_copy(kind, k).wait_send()
    for step in range(last):
        for way in range(2):

            @pl.when(ag_sends(way, step))
            def _():
                ag_copy(way, step).wait_send()

            @pl.when(rs_sends(way, step))
            def _():
                rs_copy(way, step).wait_send()


def gathered_plan(
    tokens,
    norm_gain,
    routes,
    gates,
    expert_gate,
    expert_up,
    expert_down,
    shared_gate,
    shared_up,
    shared_down,
):
    rows, width = tokens.shape
    groups = lax.axis_size("ep")
    line = groups // 2
    half = expert_gate.shape[2]
    shared_width = shared_gate.shape[1]
    ep = lax.axis_index("ep")
    own = jnp.arange(groups, dtype=jnp.int32)
    weights = jnp.sum(
        jnp.where(routes[:, :, None] == own[None, None, :], gates[:, :, None], 0.0), axis=1
    )
    everyone = lax.all_gather(weights.T, "ep").reshape(line, 2, groups, rows)
    mine = lax.dynamic_index_in_dim(everyone, ep % 2, 1, keepdims=False)
    first = lax.dynamic_index_in_dim(mine, ep, 1, keepdims=False)
    second = lax.dynamic_index_in_dim(mine, ep // 2 * 2 + 1 - ep % 2, 1, keepdims=False)
    wcol = jnp.stack([first, second], axis=2)
    any_spec = pl.BlockSpec(memory_space=pl.ANY)
    vmem_spec = pl.BlockSpec(memory_space=pltpu.VMEM)
    bf16 = jnp.bfloat16
    steps = line - 1
    return pl.pallas_call(
        functools.partial(exchange_kernel, line),
        out_shape=jax.ShapeDtypeStruct((rows, width), bf16),
        in_specs=[any_spec, vmem_spec, vmem_spec] + [any_spec] * 6,
        out_specs=vmem_spec,
        scratch_shapes=[
            pltpu.VMEM((line, rows, width), bf16),
            pltpu.VMEM((4, width, half), bf16),
            pltpu.VMEM((4, width, half), bf16),
            pltpu.VMEM((4 * half, width), bf16),
            pltpu.VMEM((width, shared_width), bf16),
            pltpu.VMEM((width, shared_width), bf16),
            pltpu.VMEM((shared_width, width), bf16),
            pltpu.VMEM((rows, width), bf16),
            pltpu.VMEM((rows, max(4 * half, shared_width)), bf16),
            pltpu.VMEM((rows, width), jnp.float32),
            pltpu.VMEM((2, steps, rows, width), bf16),
            pltpu.VMEM((2, steps, rows, width), bf16),
            pltpu.SemaphoreType.DMA((7,)),
            pltpu.SemaphoreType.DMA((2, steps)),
            pltpu.SemaphoreType.DMA((2, steps)),
            pltpu.SemaphoreType.DMA((5, 3)),
            pltpu.SemaphoreType.DMA((5, 3)),
            pltpu.SemaphoreType.DMA((2, steps)),
            pltpu.SemaphoreType.DMA((2, steps)),
        ],
        compiler_params=pltpu.CompilerParams(
            collective_id=0, has_side_effects=True, vmem_limit_bytes=56 * 1024 * 1024
        ),
    )(
        tokens,
        norm_gain.reshape(1, width),
        wcol,
        expert_gate[0],
        expert_up[0],
        expert_down[0],
        shared_gate,
        shared_up,
        shared_down,
    )


def routed_plan(
    tokens,
    norm_gain,
    routes,
    gates,
    expert_gate,
    expert_up,
    expert_down,
    shared_gate,
    shared_up,
    shared_down,
):
    token_rows, width = tokens.shape
    top_count = routes.shape[1]
    local_experts = expert_gate.shape[0]
    groups = lax.axis_size("ep")
    experts = local_experts * groups
    capacity = 3 * token_rows * top_count // (2 * experts)
    values = tokens.astype(jnp.float32)
    scaling = lax.rsqrt(jnp.mean(values * values, axis=1, keepdims=True) + 1e-06)
    normed = (values * scaling * norm_gain[None, :]).astype(jnp.bfloat16)
    flat_routes = routes.reshape(-1)
    copies = flat_routes.shape[0]
    onehot = (flat_routes[:, None] == jnp.arange(experts, dtype=jnp.int32)[None, :]).astype(
        jnp.int32
    )
    earlier = jnp.cumsum(onehot, axis=0) - onehot
    slot_index = jnp.sum(earlier * onehot, axis=1)
    buffer_row = flat_routes * capacity + slot_index
    source_token = jnp.arange(copies, dtype=jnp.int32) // top_count
    slot_token = (
        jnp.full((experts * capacity,), token_rows, jnp.int32).at[buffer_row].set(source_token)
    )
    padded = jnp.concatenate([normed, jnp.zeros((1, width), jnp.bfloat16)], axis=0)
    outgoing = padded[slot_token].reshape(groups, local_experts, capacity, width)
    whole_gate, whole_up = (
        lax.all_gather(expert_gate, "tp", axis=2, tiled=True),
        lax.all_gather(expert_up, "tp", axis=2, tiled=True),
    )
    whole_down = lax.all_gather(expert_down, "tp", axis=1, tiled=True)
    received = lax.all_to_all(outgoing, "ep", split_axis=0, concat_axis=0, tiled=True)
    gate_values = jnp.einsum(
        "secd,edf->secf", received, whole_gate, preferred_element_type=jnp.float32
    )
    up_values = jnp.einsum("secd,edf->secf", received, whole_up, preferred_element_type=jnp.float32)
    hidden = (jax.nn.silu(gate_values) * up_values).astype(jnp.bfloat16)
    summed = jnp.einsum("secf,efd->secd", hidden, whole_down, preferred_element_type=jnp.float32)
    returned = lax.all_to_all(
        summed.astype(jnp.bfloat16), "ep", split_axis=0, concat_axis=0, tiled=True
    )
    shared_hidden = (
        jax.nn.silu(jnp.dot(normed, shared_gate, preferred_element_type=jnp.float32))
        * jnp.dot(normed, shared_up, preferred_element_type=jnp.float32)
    ).astype(jnp.bfloat16)
    shared_out = jnp.dot(shared_hidden, shared_down, preferred_element_type=jnp.float32)
    flat_back = returned.reshape(experts * capacity, width)
    picked = flat_back[buffer_row].reshape(token_rows, top_count, width)
    routed = jnp.einsum("tkd,tk->td", picked.astype(jnp.float32), gates)
    return (shared_out + routed).astype(jnp.bfloat16)


def on_device(*args):
    experts = args[4].shape[0] * lax.axis_size("ep")
    paired = lax.axis_size("grp") == 2 and lax.axis_size("tp") == 2
    if paired and args[4].shape[0] == 1 and experts % 2 == 0 and experts <= 4 * args[2].shape[1]:
        return gathered_plan(*args)
    return routed_plan(*args)


def solution(mesh):
    return jax.shard_map(
        on_device,
        mesh=mesh,
        in_specs=(
            P(("grp", "ep", "tp"), None),
            P(),
            P(("grp", "ep", "tp"), None),
            P(("grp", "ep", "tp"), None),
            P("ep", None, "tp"),
            P("ep", None, "tp"),
            P("ep", "tp", None),
            P(),
            P(),
            P(),
        ),
        out_specs=P(("grp", "ep", "tp"), None),
        check_vma=False,
    )
```

```python
import functools

import jax
import jax.numpy as jnp
from jax import lax
from jax.experimental import pallas as pl
from jax.experimental.pallas import tpu as pltpu
from jax.sharding import PartitionSpec as P

MESH = pl.DeviceIdType.MESH
halves = 2


def exchange_kernel(
    tok,
    gain,
    gate_rows,
    eg,
    eu,
    ed,
    sg,
    su,
    sd,
    out,
    gathered,
    gate_of,
    G,
    U,
    D,
    SG,
    SU,
    SD,
    xn,
    hid,
    acc,
    stage,
    land,
    loc_sem,
    ag_send,
    ag_recv,
    agw_send,
    agw_recv,
    w_send,
    w_recv,
    rs_send,
    rs_recv,
):
    rows, width = tok.shape
    half = eg.shape[1]
    shared_width = sg.shape[1]
    last = gathered.shape[0] - 1
    ep = lax.axis_index("ep")
    z, y = ep // 2, ep % 2
    c = lax.axis_index("tp")
    g = lax.axis_index("grp")
    to_next, to_prev = {"ep": ep + 2}, {"ep": ep - 2}
    to_pair = {"ep": z * 2 + (1 - y)}
    to_core = {"tp": 1 - c}
    to_grp = {"grp": 1 - g}

    barrier = pltpu.get_barrier_semaphore()
    for peer in (to_pair, to_core, to_grp):
        pl.semaphore_signal(barrier, inc=1, device_id=peer, device_id_type=MESH)

    @pl.when(z < last)
    def _():
        pl.semaphore_signal(barrier, inc=1, device_id=to_next, device_id_type=MESH)

    @pl.when(z > 0)
    def _():
        pl.semaphore_signal(barrier, inc=1, device_id=to_prev, device_id_type=MESH)

    locals_ = [
        pltpu.make_async_copy(tok, gathered.at[z], loc_sem.at[0]),
        pltpu.make_async_copy(sg, SG, loc_sem.at[1]),
        pltpu.make_async_copy(su, SU, loc_sem.at[2]),
        pltpu.make_async_copy(sd, SD, loc_sem.at[3]),
        pltpu.make_async_copy(eg, G.at[0], loc_sem.at[4]),
        pltpu.make_async_copy(eu, U.at[0], loc_sem.at[5]),
        pltpu.make_async_copy(ed, D.at[pl.ds(0, half)], loc_sem.at[6]),
        pltpu.make_async_copy(gate_rows, gate_of.at[z], loc_sem.at[7]),
    ]
    for copy in locals_:
        copy.start()
    between = jnp.logical_and(z > 0, z < last)

    @pl.when(between)
    def _():
        pl.semaphore_wait(barrier, 5)

    @pl.when(jnp.logical_not(between))
    def _():
        pl.semaphore_wait(barrier, 4)

    def remote(src, dst, send, recv, peer):
        return pltpu.make_async_remote_copy(
            src_ref=src,
            dst_ref=dst,
            send_sem=send,
            recv_sem=recv,
            device_id=peer,
            device_id_type=MESH,
        )

    def ag_copies(way, step):
        block = z - step if way == 0 else z + step
        peer = to_next if way == 0 else to_prev
        return [
            remote(src if step == 0 else dst.at[block], dst.at[block], a, b, peer)
            for src, dst, a, b in (
                (gate_rows, gate_of, agw_send.at[way, step], agw_recv.at[way, step]),
                (tok, gathered, ag_send.at[way, step], ag_recv.at[way, step]),
            )
        ]

    def ag_sends(way, step):
        if way == 0:
            return jnp.logical_and(z - step >= 0, z < last)
        return jnp.logical_and(z + step <= last, z > 0)

    def ag_arrivals(way, step):
        block = z - 1 - step if way == 0 else z + 1 + step
        peer = to_next if way == 0 else to_prev
        return [
            remote(dst.at[block], dst.at[block], a, b, peer)
            for dst, a, b in (
                (gate_of, agw_send.at[way, step], agw_recv.at[way, step]),
                (gathered, ag_send.at[way, step], ag_recv.at[way, step]),
            )
        ]

    def ag_arrives(way, step):
        return z - 1 - step >= 0 if way == 0 else z + 1 + step <= last

    def ag_start(step):
        for way in range(2):

            @pl.when(ag_sends(way, step))
            def _():
                for copy in ag_copies(way, step):
                    copy.start()

    def ag_wait(step):
        for way in range(2):

            @pl.when(ag_arrives(way, step))
            def _():
                for copy in ag_arrivals(way, step):
                    copy.wait_recv()

    def piece(k, unit, part):
        if k == 2:
            if part is None:
                return D.at[pl.ds(unit * half, half)]
            n = half // 2
            return D.at[pl.ds(pl.multiple_of(unit * half + part * n, n), n)]
        whole = (G, U)[k].at[unit]
        if part is None:
            return whole
        n = width // 2
        return whole.at[pl.ds(pl.multiple_of(part * n, n), n)]

    own = (eg, eu, ed)

    def own_part(k):
        n = own[k].shape[0] // 2
        return own[k].at[pl.ds(pl.multiple_of(g * n, n), n)]

    def w_copy(kind, k):
        sems = (w_send.at[kind, k], w_recv.at[kind, k])
        if kind == 0:
            return remote(own[k], piece(k, 1, None), *sems, to_core)
        if kind == 1:
            return remote(own_part(k), piece(k, 2, g), *sems, to_pair)
        if kind == 2:
            return remote(piece(k, 2, g), piece(k, 2, g), *sems, to_grp)
        if kind == 3:
            return remote(piece(k, 2, g), piece(k, 3, g), *sems, to_core)
        return remote(piece(k, 2, 1 - g), piece(k, 3, 1 - g), *sems, to_core)

    def w_arrival(kind, k):
        if kind != 2:
            return w_copy(kind, k)
        slot = piece(k, 2, 1 - g)
        return remote(slot, slot, w_send.at[kind, k], w_recv.at[kind, k], to_grp)

    ag_start(0)
    for k in range(3):
        w_copy(1, k).start()
    for k in range(3):
        w_copy(0, k).start()

    tile = 32

    def normalise(block):
        @pl.loop(0, rows // tile)
        def _(i):
            part = pl.ds(pl.multiple_of(i * tile, tile), tile)
            values = gathered[block, part, :].astype(jnp.float32)
            scaling = lax.rsqrt(jnp.mean(values * values, axis=1, keepdims=True) + 1e-06)
            xn[part, :] = (values * scaling * gain[...]).astype(jnp.bfloat16)

    def act(a, b):
        return a / (1.0 + jnp.exp(-a)) * b

    cols_n = 512 if width % 512 == 0 else width

    def over_columns(fn):
        @pl.loop(0, width // cols_n)
        def _(i):
            fn(pl.ds(pl.multiple_of(i * cols_n, cols_n), cols_n))

    def routed(block, fn):
        normalise(block)
        columns = jnp.transpose(gate_of[block])
        named = lax.broadcasted_iota(jnp.int32, columns.shape, 1)

        @pl.loop(0, 4)
        def _(u):
            a = jnp.dot(xn[...], G[u], preferred_element_type=jnp.float32)
            b = jnp.dot(xn[...], U[u], preferred_element_type=jnp.float32)
            expert = 2 * z + (y + u // 2) % 2
            w = jnp.sum(jnp.where(named == expert, columns, 0.0), axis=1, keepdims=True)
            hid[:, pl.ds(pl.multiple_of(u * half, half), half)] = (act(a, b) * w).astype(
                jnp.bfloat16
            )

        over_columns(
            lambda cols: fn(
                cols,
                jnp.dot(
                    hid[:, 0 : 4 * half], D[:, cols], preferred_element_type=jnp.float32
                ),
            )
        )

    locals_[0].wait()
    locals_[7].wait()
    normalise(z)
    for copy in locals_[1:4]:
        copy.wait()

    @pl.loop(0, shared_width // half)
    def _(u):
        part = pl.ds(pl.multiple_of(u * half, half), half)
        a = jnp.dot(xn[...], SG[:, part], preferred_element_type=jnp.float32)
        b = jnp.dot(xn[...], SU[:, part], preferred_element_type=jnp.float32)
        hid[:, part] = act(a, b).astype(jnp.bfloat16)

    def shared_store(cols):
        acc[:, cols] = jnp.dot(
            hid[:, 0:shared_width], SD[:, cols], preferred_element_type=jnp.float32
        )

    over_columns(shared_store)

    def pass_on(k):
        w_arrival(1, k).wait_recv()
        w_copy(2, k).start()
        w_copy(3, k).start()

    def pass_over(k):
        w_arrival(2, k).wait_recv()
        w_copy(4, k).start()

    pass_on(0)
    pass_on(1)
    ag_wait(0)
    ag_start(1)
    pass_over(0)
    pass_on(2)
    ag_wait(1)
    ag_start(2)
    pass_over(1)
    pass_over(2)
    for copy in locals_[4:7]:
        copy.wait()
    for kind in (0, 3, 4):
        for k in range(3):
            w_arrival(kind, k).wait_recv()

    near, side = z // 2, z % 2
    dest = (2 - near, last * (1 - near), z + 1 - 2 * side)
    ways = (near, near, side)
    piece_rows = rows // halves

    def part_of(h):
        return pl.ds(h * piece_rows, piece_rows)

    def rs_copy(i, h):
        peer = {"ep": ep + 2 - 4 * ways[i]}
        return remote(
            stage.at[i, part_of(h)],
            land.at[ways[i], dest[i], part_of(h)],
            rs_send.at[i, h],
            rs_recv.at[ways[i], dest[i], h],
            peer,
        )

    def rs_arrival(way, block, h):
        slot = land.at[way, block, part_of(h)]
        return remote(slot, slot, rs_send.at[0, h], rs_recv.at[way, block, h], to_pair)

    def over_rows(h, fn):
        @pl.loop(0, piece_rows // tile)
        def _(i):
            fn(pl.ds(pl.multiple_of(h * piece_rows + i * tile, tile), tile))

    def partial(i):
        def store(cols, value):
            stage[i, :, cols] = value.astype(jnp.bfloat16)

        routed(dest[i], store)

    def send_first(i):
        @pl.when(jnp.logical_not(between))
        def _():
            for h in range(halves):
                rs_copy(i, h).start()

    def send_sum(i):
        @pl.when(between)
        def _():
            for h in range(halves):
                rs_arrival(ways[i], dest[i], h).wait_recv()

                def add(part):
                    stage[i, part, :] = (
                        stage[i, part, :].astype(jnp.float32)
                        + land[ways[i], dest[i], part, :].astype(jnp.float32)
                    ).astype(jnp.bfloat16)

                over_rows(h, add)
                rs_copy(i, h).start()

    partial(0)
    send_first(0)
    ag_wait(2)
    partial(1)
    send_first(1)
    send_sum(0)
    partial(2)
    send_first(2)
    send_sum(1)
    send_sum(2)

    def add_own(cols, value):
        acc[:, cols] += value

    routed(z, add_own)

    for h in range(halves):
        for way in range(2):

            @pl.when(z > 0 if way == 0 else z < last)
            def _():
                rs_arrival(way, z, h).wait_recv()

                def add(part):
                    acc[part, :] += land[way, z, part, :].astype(jnp.float32)

                over_rows(h, add)

        def finish(part):
            out[part, :] = acc[part, :].astype(jnp.bfloat16)

        over_rows(h, finish)

    for kind in range(5):
        for k in range(3):
            w_copy(kind, k).wait_send()
    for i in range(3):
        for h in range(halves):
            rs_copy(i, h).wait_send()
    for step in range(last):
        for way in range(2):

            @pl.when(ag_sends(way, step))
            def _():
                for copy in ag_copies(way, step):
                    copy.wait_send()


def gathered_plan(
    tokens,
    norm_gain,
    routes,
    gates,
    expert_gate,
    expert_up,
    expert_down,
    shared_gate,
    shared_up,
    shared_down,
):
    rows, width = tokens.shape
    groups = lax.axis_size("ep")
    line = groups // 2
    half = expert_gate.shape[2]
    shared_width = shared_gate.shape[1]
    own = jnp.arange(groups, dtype=jnp.int32)
    weights = jnp.sum(
        jnp.where(routes[:, :, None] == own[None, None, :], gates[:, :, None], 0.0), axis=1
    )
    gate_rows = jnp.pad(weights.T, ((0, -groups % 8), (0, 0)))
    any_spec = pl.BlockSpec(memory_space=pl.ANY)
    vmem_spec = pl.BlockSpec(memory_space=pltpu.VMEM)
    bf16 = jnp.bfloat16
    steps = line - 1
    return pl.pallas_call(
        exchange_kernel,
        out_shape=jax.ShapeDtypeStruct((rows, width), bf16),
        in_specs=[any_spec, vmem_spec] + [any_spec] * 7,
        out_specs=vmem_spec,
        scratch_shapes=[
            pltpu.VMEM((line, rows, width), bf16),
            pltpu.VMEM((line,) + gate_rows.shape, jnp.float32),
            pltpu.VMEM((4, width, half), bf16),
            pltpu.VMEM((4, width, half), bf16),
            pltpu.VMEM((4 * half, width), bf16),
            pltpu.VMEM((width, shared_width), bf16),
            pltpu.VMEM((width, shared_width), bf16),
            pltpu.VMEM((shared_width, width), bf16),
            pltpu.VMEM((rows, width), bf16),
            pltpu.VMEM((rows, max(4 * half, shared_width)), bf16),
            pltpu.VMEM((rows, width), jnp.float32),
            pltpu.VMEM((steps, rows, width), bf16),
            pltpu.VMEM((2, line, rows, width), bf16),
            pltpu.SemaphoreType.DMA((8,)),
            pltpu.SemaphoreType.DMA((2, steps)),
            pltpu.SemaphoreType.DMA((2, steps)),
            pltpu.SemaphoreType.DMA((2, steps)),
            pltpu.SemaphoreType.DMA((2, steps)),
            pltpu.SemaphoreType.DMA((5, 3)),
            pltpu.SemaphoreType.DMA((5, 3)),
            pltpu.SemaphoreType.DMA((steps, halves)),
            pltpu.SemaphoreType.DMA((2, line, halves)),
        ],
        compiler_params=pltpu.CompilerParams(
            collective_id=0, has_side_effects=True, vmem_limit_bytes=56 * 1024 * 1024
        ),
    )(
        tokens,
        norm_gain.reshape(1, width),
        gate_rows,
        expert_gate[0],
        expert_up[0],
        expert_down[0],
        shared_gate,
        shared_up,
        shared_down,
    )


def routed_plan(
    tokens,
    norm_gain,
    routes,
    gates,
    expert_gate,
    expert_up,
    expert_down,
    shared_gate,
    shared_up,
    shared_down,
):
    token_rows, width = tokens.shape
    top_count = routes.shape[1]
    local_experts = expert_gate.shape[0]
    groups = lax.axis_size("ep")
    experts = local_experts * groups
    capacity = 3 * token_rows * top_count // (2 * experts)
    values = tokens.astype(jnp.float32)
    scaling = lax.rsqrt(jnp.mean(values * values, axis=1, keepdims=True) + 1e-06)
    normed = (values * scaling * norm_gain[None, :]).astype(jnp.bfloat16)
    flat_routes = routes.reshape(-1)
    copies = flat_routes.shape[0]
    onehot = (flat_routes[:, None] == jnp.arange(experts, dtype=jnp.int32)[None, :]).astype(
        jnp.int32
    )
    earlier = jnp.cumsum(onehot, axis=0) - onehot
    slot_index = jnp.sum(earlier * onehot, axis=1)
    buffer_row = flat_routes * capacity + slot_index
    source_token = jnp.arange(copies, dtype=jnp.int32) // top_count
    slot_token = (
        jnp.full((experts * capacity,), token_rows, jnp.int32).at[buffer_row].set(source_token)
    )
    padded = jnp.concatenate([normed, jnp.zeros((1, width), jnp.bfloat16)], axis=0)
    outgoing = padded[slot_token].reshape(groups, local_experts, capacity, width)
    whole_gate, whole_up = (
        lax.all_gather(expert_gate, "tp", axis=2, tiled=True),
        lax.all_gather(expert_up, "tp", axis=2, tiled=True),
    )
    whole_down = lax.all_gather(expert_down, "tp", axis=1, tiled=True)
    received = lax.all_to_all(outgoing, "ep", split_axis=0, concat_axis=0, tiled=True)
    gate_values = jnp.einsum(
        "secd,edf->secf", received, whole_gate, preferred_element_type=jnp.float32
    )
    up_values = jnp.einsum("secd,edf->secf", received, whole_up, preferred_element_type=jnp.float32)
    hidden = (jax.nn.silu(gate_values) * up_values).astype(jnp.bfloat16)
    summed = jnp.einsum("secf,efd->secd", hidden, whole_down, preferred_element_type=jnp.float32)
    returned = lax.all_to_all(
        summed.astype(jnp.bfloat16), "ep", split_axis=0, concat_axis=0, tiled=True
    )
    shared_hidden = (
        jax.nn.silu(jnp.dot(normed, shared_gate, preferred_element_type=jnp.float32))
        * jnp.dot(normed, shared_up, preferred_element_type=jnp.float32)
    ).astype(jnp.bfloat16)
    shared_out = jnp.dot(shared_hidden, shared_down, preferred_element_type=jnp.float32)
    flat_back = returned.reshape(experts * capacity, width)
    picked = flat_back[buffer_row].reshape(token_rows, top_count, width)
    routed = jnp.einsum("tkd,tk->td", picked.astype(jnp.float32), gates)
    return (shared_out + routed).astype(jnp.bfloat16)


def on_device(*args):
    experts = args[4].shape[0] * lax.axis_size("ep")
    paired = lax.axis_size("grp") == 2 and lax.axis_size("tp") == 2 and args[4].shape[0] == 1
    if paired and experts == 2 * 4 and experts <= 4 * args[2].shape[1]:
        return gathered_plan(*args)
    return routed_plan(*args)


def solution(mesh):
    return jax.shard_map(
        on_device,
        mesh=mesh,
        in_specs=(
            P(("grp", "ep", "tp"), None),
            P(),
            P(("grp", "ep", "tp"), None),
            P(("grp", "ep", "tp"), None),
            P("ep", None, "tp"),
            P("ep", None, "tp"),
            P("ep", "tp", None),
            P(),
            P(),
            P(),
        ),
        out_specs=P(("grp", "ep", "tp"), None),
        check_vma=False,
    )
```

```python
import functools

import jax
import jax.numpy as jnp
from jax import lax
from jax.experimental import pallas as pl
from jax.experimental.pallas import tpu as pltpu
from jax.sharding import PartitionSpec as P

MESH = pl.DeviceIdType.MESH
pieces = 4


def exchange_kernel(
    tok,
    gain,
    gate_rows,
    eg,
    eu,
    ed,
    sg,
    su,
    sd,
    out,
    gathered,
    gate_of,
    G,
    U,
    D,
    SG,
    SU,
    SD,
    xn,
    hid,
    acc,
    stage,
    land,
    loc_sem,
    ag_send,
    ag_recv,
    agw_send,
    agw_recv,
    w_send,
    w_recv,
    rs_send,
    rs_recv,
):
    rows, width = tok.shape
    half = eg.shape[1]
    shared_width = sg.shape[1]
    last = gathered.shape[0] - 1
    ep = lax.axis_index("ep")
    z, y = ep // 2, ep % 2
    c = lax.axis_index("tp")
    g = lax.axis_index("grp")
    to_next, to_prev = {"ep": ep + 2}, {"ep": ep - 2}
    to_pair = {"ep": z * 2 + (1 - y)}
    to_core = {"tp": 1 - c}
    to_grp = {"grp": 1 - g}

    barrier = pltpu.get_barrier_semaphore()
    for peer in (to_pair, to_core, to_grp):
        pl.semaphore_signal(barrier, inc=1, device_id=peer, device_id_type=MESH)

    @pl.when(z < last)
    def _():
        pl.semaphore_signal(barrier, inc=1, device_id=to_next, device_id_type=MESH)

    @pl.when(z > 0)
    def _():
        pl.semaphore_signal(barrier, inc=1, device_id=to_prev, device_id_type=MESH)

    locals_ = [
        pltpu.make_async_copy(tok, gathered.at[z], loc_sem.at[0]),
        pltpu.make_async_copy(sg, SG, loc_sem.at[1]),
        pltpu.make_async_copy(su, SU, loc_sem.at[2]),
        pltpu.make_async_copy(sd, SD, loc_sem.at[3]),
        pltpu.make_async_copy(eg, G.at[0], loc_sem.at[4]),
        pltpu.make_async_copy(eu, U.at[0], loc_sem.at[5]),
        pltpu.make_async_copy(ed, D.at[pl.ds(0, half)], loc_sem.at[6]),
        pltpu.make_async_copy(gate_rows, gate_of.at[z], loc_sem.at[7]),
    ]
    for copy in locals_:
        copy.start()
    between = jnp.logical_and(z > 0, z < last)

    @pl.when(between)
    def _():
        pl.semaphore_wait(barrier, 5)

    @pl.when(jnp.logical_not(between))
    def _():
        pl.semaphore_wait(barrier, 4)

    def remote(src, dst, send, recv, peer):
        return pltpu.make_async_remote_copy(
            src_ref=src,
            dst_ref=dst,
            send_sem=send,
            recv_sem=recv,
            device_id=peer,
            device_id_type=MESH,
        )

    def ag_copies(way, step):
        block = z - step if way == 0 else z + step
        peer = to_next if way == 0 else to_prev
        return [
            remote(src if step == 0 else dst.at[block], dst.at[block], a, b, peer)
            for src, dst, a, b in (
                (gate_rows, gate_of, agw_send.at[way, step], agw_recv.at[way, step]),
                (tok, gathered, ag_send.at[way, step], ag_recv.at[way, step]),
            )
        ]

    def ag_sends(way, step):
        if way == 0:
            return jnp.logical_and(z - step >= 0, z < last)
        return jnp.logical_and(z + step <= last, z > 0)

    def ag_arrivals(way, step):
        block = z - 1 - step if way == 0 else z + 1 + step
        peer = to_next if way == 0 else to_prev
        return [
            remote(dst.at[block], dst.at[block], a, b, peer)
            for dst, a, b in (
                (gate_of, agw_send.at[way, step], agw_recv.at[way, step]),
                (gathered, ag_send.at[way, step], ag_recv.at[way, step]),
            )
        ]

    def ag_arrives(way, step):
        return z - 1 - step >= 0 if way == 0 else z + 1 + step <= last

    def ag_start(step):
        for way in range(2):

            @pl.when(ag_sends(way, step))
            def _():
                for copy in ag_copies(way, step):
                    copy.start()

    def ag_wait(step):
        for way in range(2):

            @pl.when(ag_arrives(way, step))
            def _():
                for copy in ag_arrivals(way, step):
                    copy.wait_recv()

    own = (eg, eu, ed)

    def cut(ref, base, count, part, parts):
        n = count // parts
        return ref.at[pl.ds(pl.multiple_of(base + part * n, n), n)]

    def slot(k, unit, part, parts):
        if k // 2 == 2:
            return cut(D, unit * half, half, part, parts)
        return cut((G, U)[k // 2].at[unit], 0, width, part, parts)

    def owned(k, part, parts):
        ref = own[k // 2]
        return cut(ref, 0, ref.shape[0], part, parts)

    def w_copy(kind, k):
        sems = (w_send.at[kind, k], w_recv.at[kind, k])
        mine, theirs = 2 * g + k % 2, 2 * (1 - g) + k % 2
        if kind == 0:
            return remote(owned(k, k % 2, 2), slot(k, 1, k % 2, 2), *sems, to_core)
        if kind == 1:
            return remote(owned(k, mine, 4), slot(k, 2, mine, 4), *sems, to_pair)
        if kind == 2:
            return remote(slot(k, 2, mine, 4), slot(k, 2, mine, 4), *sems, to_grp)
        if kind == 3:
            return remote(slot(k, 2, mine, 4), slot(k, 3, mine, 4), *sems, to_core)
        return remote(slot(k, 2, theirs, 4), slot(k, 3, theirs, 4), *sems, to_core)

    def w_arrival(kind, k):
        if kind != 2:
            return w_copy(kind, k)
        place = slot(k, 2, 2 * (1 - g) + k % 2, 4)
        return remote(place, place, w_send.at[kind, k], w_recv.at[kind, k], to_grp)

    ag_start(0)
    for k in range(6):
        w_copy(1, k).start()
    for k in range(6):
        w_copy(0, k).start()

    tile = 32

    def normalise(block):
        @pl.loop(0, rows // tile)
        def _(i):
            part = pl.ds(pl.multiple_of(i * tile, tile), tile)
            values = gathered[block, part, :].astype(jnp.float32)
            scaling = lax.rsqrt(jnp.mean(values * values, axis=1, keepdims=True) + 1e-06)
            xn[part, :] = (values * scaling * gain[...]).astype(jnp.bfloat16)

    def act(a, b):
        return a / (1.0 + jnp.exp(-a)) * b

    cols_n = 512 if width % 512 == 0 else width

    def over_columns(fn):
        @pl.loop(0, width // cols_n)
        def _(i):
            fn(pl.ds(pl.multiple_of(i * cols_n, cols_n), cols_n))

    def routed(block, fn):
        normalise(block)
        columns = jnp.transpose(gate_of[block])
        named = lax.broadcasted_iota(jnp.int32, columns.shape, 1)

        @pl.loop(0, 4)
        def _(u):
            a = jnp.dot(xn[...], G[u], preferred_element_type=jnp.float32)
            b = jnp.dot(xn[...], U[u], preferred_element_type=jnp.float32)
            expert = 2 * z + (y + u // 2) % 2
            w = jnp.sum(jnp.where(named == expert, columns, 0.0), axis=1, keepdims=True)
            hid[:, pl.ds(pl.multiple_of(u * half, half), half)] = (act(a, b) * w).astype(
                jnp.bfloat16
            )

        over_columns(
            lambda cols: fn(
                cols,
                jnp.dot(
                    hid[:, 0 : 4 * half], D[:, cols], preferred_element_type=jnp.float32
                ),
            )
        )

    locals_[0].wait()
    locals_[7].wait()
    normalise(z)
    for copy in locals_[1:4]:
        copy.wait()

    @pl.loop(0, shared_width // half)
    def _(u):
        part = pl.ds(pl.multiple_of(u * half, half), half)
        a = jnp.dot(xn[...], SG[:, part], preferred_element_type=jnp.float32)
        b = jnp.dot(xn[...], SU[:, part], preferred_element_type=jnp.float32)
        hid[:, part] = act(a, b).astype(jnp.bfloat16)

    def shared_store(cols):
        acc[:, cols] = jnp.dot(
            hid[:, 0:shared_width], SD[:, cols], preferred_element_type=jnp.float32
        )

    over_columns(shared_store)

    def pass_on(k):
        w_arrival(1, k).wait_recv()
        w_copy(2, k).start()
        w_copy(3, k).start()

    def pass_over(k):
        w_arrival(2, k).wait_recv()
        w_copy(4, k).start()

    pass_on(0)
    pass_on(1)
    pass_over(0)
    pass_on(2)
    pass_over(1)
    pass_on(3)
    ag_wait(0)
    ag_start(1)
    pass_over(2)
    pass_on(4)
    pass_over(3)
    pass_on(5)
    pass_over(4)
    pass_over(5)
    for copy in locals_[4:7]:
        copy.wait()
    for kind in (0, 3, 4):
        for k in range(6):
            w_arrival(kind, k).wait_recv()
    ag_wait(1)
    ag_start(2)

    near, side = z // 2, z % 2
    dest = (2 - near, last * (1 - near), z + 1 - 2 * side)
    ways = (near, near, side)
    piece_rows = rows // pieces

    def part_of(h):
        return pl.ds(h * piece_rows, piece_rows)

    def rs_copy(i, h):
        peer = {"ep": ep + 2 - 4 * ways[i]}
        return remote(
            stage.at[i, part_of(h)],
            land.at[ways[i], dest[i], part_of(h)],
            rs_send.at[i, h],
            rs_recv.at[ways[i], dest[i], h],
            peer,
        )

    def rs_arrival(way, block, h):
        slot = land.at[way, block, part_of(h)]
        return remote(slot, slot, rs_send.at[0, h], rs_recv.at[way, block, h], to_pair)

    def over_rows(h, fn):
        @pl.loop(0, piece_rows // tile)
        def _(i):
            fn(pl.ds(pl.multiple_of(h * piece_rows + i * tile, tile), tile))

    def partial(i):
        def store(cols, value):
            stage[i, :, cols] = value.astype(jnp.bfloat16)

        routed(dest[i], store)

    def send_first(i):
        @pl.when(jnp.logical_not(between))
        def _():
            for h in range(pieces):
                rs_copy(i, h).start()

    def send_sum(i):
        @pl.when(between)
        def _():
            for h in range(pieces):
                rs_arrival(ways[i], dest[i], h).wait_recv()

                def add(part):
                    stage[i, part, :] = (
                        stage[i, part, :].astype(jnp.float32)
                        + land[ways[i], dest[i], part, :].astype(jnp.float32)
                    ).astype(jnp.bfloat16)

                over_rows(h, add)
                rs_copy(i, h).start()

    partial(0)
    send_first(0)
    ag_wait(2)
    partial(1)
    send_first(1)
    send_sum(0)
    partial(2)
    send_first(2)
    send_sum(1)
    send_sum(2)

    def add_own(cols, value):
        acc[:, cols] += value

    routed(z, add_own)

    for h in range(pieces):
        for way in range(2):

            @pl.when(z > 0 if way == 0 else z < last)
            def _():
                rs_arrival(way, z, h).wait_recv()

                def add(part):
                    acc[part, :] += land[way, z, part, :].astype(jnp.float32)

                over_rows(h, add)

        def finish(part):
            out[part, :] = acc[part, :].astype(jnp.bfloat16)

        over_rows(h, finish)

    for kind in range(5):
        for k in range(6):
            w_copy(kind, k).wait_send()
    for i in range(3):
        for h in range(pieces):
            rs_copy(i, h).wait_send()
    for step in range(last):
        for way in range(2):

            @pl.when(ag_sends(way, step))
            def _():
                for copy in ag_copies(way, step):
                    copy.wait_send()


def gathered_plan(
    tokens,
    norm_gain,
    routes,
    gates,
    expert_gate,
    expert_up,
    expert_down,
    shared_gate,
    shared_up,
    shared_down,
):
    rows, width = tokens.shape
    groups = lax.axis_size("ep")
    line = groups // 2
    half = expert_gate.shape[2]
    shared_width = shared_gate.shape[1]
    own = jnp.arange(groups, dtype=jnp.int32)
    weights = jnp.sum(
        jnp.where(routes[:, :, None] == own[None, None, :], gates[:, :, None], 0.0), axis=1
    )
    gate_rows = jnp.pad(weights.T, ((0, -groups % 8), (0, 0)))
    any_spec = pl.BlockSpec(memory_space=pl.ANY)
    vmem_spec = pl.BlockSpec(memory_space=pltpu.VMEM)
    bf16 = jnp.bfloat16
    steps = line - 1
    return pl.pallas_call(
        exchange_kernel,
        out_shape=jax.ShapeDtypeStruct((rows, width), bf16),
        in_specs=[any_spec, vmem_spec] + [any_spec] * 7,
        out_specs=vmem_spec,
        scratch_shapes=[
            pltpu.VMEM((line, rows, width), bf16),
            pltpu.VMEM((line,) + gate_rows.shape, jnp.float32),
            pltpu.VMEM((4, width, half), bf16),
            pltpu.VMEM((4, width, half), bf16),
            pltpu.VMEM((4 * half, width), bf16),
            pltpu.VMEM((width, shared_width), bf16),
            pltpu.VMEM((width, shared_width), bf16),
            pltpu.VMEM((shared_width, width), bf16),
            pltpu.VMEM((rows, width), bf16),
            pltpu.VMEM((rows, max(4 * half, shared_width)), bf16),
            pltpu.VMEM((rows, width), jnp.float32),
            pltpu.VMEM((steps, rows, width), bf16),
            pltpu.VMEM((2, line, rows, width), bf16),
            pltpu.SemaphoreType.DMA((8,)),
            pltpu.SemaphoreType.DMA((2, steps)),
            pltpu.SemaphoreType.DMA((2, steps)),
            pltpu.SemaphoreType.DMA((2, steps)),
            pltpu.SemaphoreType.DMA((2, steps)),
            pltpu.SemaphoreType.DMA((5, 6)),
            pltpu.SemaphoreType.DMA((5, 6)),
            pltpu.SemaphoreType.DMA((steps, pieces)),
            pltpu.SemaphoreType.DMA((2, line, pieces)),
        ],
        compiler_params=pltpu.CompilerParams(
            collective_id=0, has_side_effects=True, vmem_limit_bytes=56 * 1024 * 1024
        ),
    )(
        tokens,
        norm_gain.reshape(1, width),
        gate_rows,
        expert_gate[0],
        expert_up[0],
        expert_down[0],
        shared_gate,
        shared_up,
        shared_down,
    )


def routed_plan(
    tokens,
    norm_gain,
    routes,
    gates,
    expert_gate,
    expert_up,
    expert_down,
    shared_gate,
    shared_up,
    shared_down,
):
    token_rows, width = tokens.shape
    top_count = routes.shape[1]
    local_experts = expert_gate.shape[0]
    groups = lax.axis_size("ep")
    experts = local_experts * groups
    capacity = 3 * token_rows * top_count // (2 * experts)
    values = tokens.astype(jnp.float32)
    scaling = lax.rsqrt(jnp.mean(values * values, axis=1, keepdims=True) + 1e-06)
    normed = (values * scaling * norm_gain[None, :]).astype(jnp.bfloat16)
    flat_routes = routes.reshape(-1)
    copies = flat_routes.shape[0]
    onehot = (flat_routes[:, None] == jnp.arange(experts, dtype=jnp.int32)[None, :]).astype(
        jnp.int32
    )
    earlier = jnp.cumsum(onehot, axis=0) - onehot
    slot_index = jnp.sum(earlier * onehot, axis=1)
    buffer_row = flat_routes * capacity + slot_index
    source_token = jnp.arange(copies, dtype=jnp.int32) // top_count
    slot_token = (
        jnp.full((experts * capacity,), token_rows, jnp.int32).at[buffer_row].set(source_token)
    )
    padded = jnp.concatenate([normed, jnp.zeros((1, width), jnp.bfloat16)], axis=0)
    outgoing = padded[slot_token].reshape(groups, local_experts, capacity, width)
    whole_gate, whole_up = (
        lax.all_gather(expert_gate, "tp", axis=2, tiled=True),
        lax.all_gather(expert_up, "tp", axis=2, tiled=True),
    )
    whole_down = lax.all_gather(expert_down, "tp", axis=1, tiled=True)
    received = lax.all_to_all(outgoing, "ep", split_axis=0, concat_axis=0, tiled=True)
    gate_values = jnp.einsum(
        "secd,edf->secf", received, whole_gate, preferred_element_type=jnp.float32
    )
    up_values = jnp.einsum("secd,edf->secf", received, whole_up, preferred_element_type=jnp.float32)
    hidden = (jax.nn.silu(gate_values) * up_values).astype(jnp.bfloat16)
    summed = jnp.einsum("secf,efd->secd", hidden, whole_down, preferred_element_type=jnp.float32)
    returned = lax.all_to_all(
        summed.astype(jnp.bfloat16), "ep", split_axis=0, concat_axis=0, tiled=True
    )
    shared_hidden = (
        jax.nn.silu(jnp.dot(normed, shared_gate, preferred_element_type=jnp.float32))
        * jnp.dot(normed, shared_up, preferred_element_type=jnp.float32)
    ).astype(jnp.bfloat16)
    shared_out = jnp.dot(shared_hidden, shared_down, preferred_element_type=jnp.float32)
    flat_back = returned.reshape(experts * capacity, width)
    picked = flat_back[buffer_row].reshape(token_rows, top_count, width)
    routed = jnp.einsum("tkd,tk->td", picked.astype(jnp.float32), gates)
    return (shared_out + routed).astype(jnp.bfloat16)


def on_device(*args):
    experts = args[4].shape[0] * lax.axis_size("ep")
    paired = lax.axis_size("grp") == 2 and lax.axis_size("tp") == 2 and args[4].shape[0] == 1
    if paired and experts == 2 * 4 and experts <= 4 * args[2].shape[1]:
        return gathered_plan(*args)
    return routed_plan(*args)


def solution(mesh):
    return jax.shard_map(
        on_device,
        mesh=mesh,
        in_specs=(
            P(("grp", "ep", "tp"), None),
            P(),
            P(("grp", "ep", "tp"), None),
            P(("grp", "ep", "tp"), None),
            P("ep", None, "tp"),
            P("ep", None, "tp"),
            P("ep", "tp", None),
            P(),
            P(),
            P(),
        ),
        out_specs=P(("grp", "ep", "tp"), None),
        check_vma=False,
    )
```
